32 devices in a mesh: sp: 8 (over z, x), tp: 4 (over y, core).
Axes of the slice: x: 2, y: 2, z: 4, core: 2. Of those that a mesh axis runs over, the one named last changes fastest.
Arguments:
- stream: bfloat16 [4096, 2048], P('sp', 'tp'), may hold values from -6 to 6
- norm_gain: float32 [2, 2048], replicated, may hold values from 0.1 to 1.9
- w_value: bfloat16 [2, 2048, 2048], P(None, 'sp', 'tp'), may hold values from -0.125 to 0.125
- w_inner: bfloat16 [2, 2048, 2048], P(None, 'sp', 'tp'), may hold values from -0.125 to 0.125
- w_outer: bfloat16 [2, 2048, 2048], P(None, 'sp', 'tp'), may hold values from -0.125 to 0.125
- conv_taps: float32 [2, 3, 2048], P(None, None, 'tp'), may hold values from -3 to 3
- w_output: bfloat16 [2, 2048, 2048], P(None, 'tp', 'sp'), may hold values from -0.125 to 0.125
Outputs:
- result: bfloat16 [4096, 2048], P('sp', 'tp')
The draws below stay inside these ranges and needn't reach their ends.
All inputs are finite; a program needn't handle non-finite values.
Results may differ from the reference program's by a relative error of at most 0.02.
Values may be sent and summed in bfloat16 or wider, within the bound.
A program may use at most 64 MiB of HBM per device.

```python
import jax
import jax.numpy as jnp
from jax import lax

D = 2048
LAYERS = 2
TAPS = 3
TOKENS = 4096
N_TP = 4


def steps_of(stream_key, dims, shards, smallest, largest):
    level, own = 1.0, jax.random.fold_in(stream_key, 6)
    for dim, shards_of in shards:
        heights = jnp.exp(jax.random.uniform(jax.random.fold_in(own, dim), (shards_of,), jnp.float32, smallest / len(shards), largest / len(shards)))
        level = level * jnp.repeat(heights, dims[dim] // shards_of).reshape([-1 if axis == dim else 1 for axis in range(len(dims))])
    return level


def bell_draw(own_key, shape, scale, limit, pieces=(), kind=jnp.bfloat16):
    factor_of = steps_of(own_key, shape, pieces, -0.22, 0.18) if pieces else 1.0
    result = jax.random.normal(own_key, shape, jnp.float32) * scale * factor_of
    return jnp.minimum(jnp.maximum(result, -limit), limit).astype(kind)


def setup_inputs(seed: int = 0) -> dict:
    seeds = jax.random.split(jax.random.key(seed), 8)
    return {
        "stream": bell_draw(seeds[0], (TOKENS, D), 1.0, 6.0, ((0, 8), (1, 4))),
        "norm_gain": jnp.clip(1.0 + 0.18 * jax.random.normal(seeds[1], (LAYERS, D), jnp.float32), 0.1, 1.9),
        "w_value": bell_draw(seeds[2], (LAYERS, D, D), D ** -0.5, 0.125, ((1, 8), (2, 4))),
        "w_inner": bell_draw(seeds[3], (LAYERS, D, D), D ** -0.5, 0.125, ((1, 8), (2, 4))),
        "w_outer": bell_draw(seeds[4], (LAYERS, D, D), D ** -0.5, 0.125, ((1, 8), (2, 4))),
        "conv_taps": bell_draw(seeds[5], (LAYERS, TAPS, D), 0.6, 3.0, ((2, 4),), jnp.float32),
        "w_output": bell_draw(seeds[6], (LAYERS, D, D), D ** -0.5, 0.125, ((1, 4), (2, 8))),
    }


EPSILON = 1e-06

def one_layer(stream_now, gain, weight_value, weight_inner, weight_outer, taps, weight_output):
    stream_float = stream_now.astype(jnp.float32)
    scale = lax.rsqrt(lax.optimization_barrier(jnp.mean(stream_float * stream_float, axis=-1, keepdims=True)) + EPSILON)
    normed = (stream_float * scale * gain).astype(jnp.bfloat16)
    value_proj = jnp.dot(normed, weight_value, preferred_element_type=jnp.float32)
    inner_gate = jnp.dot(normed, weight_inner, preferred_element_type=jnp.float32)
    outer_gate = jnp.dot(normed, weight_outer, preferred_element_type=jnp.float32)
    mixed = (inner_gate * value_proj).astype(jnp.bfloat16)
    row_count = mixed.shape[0]
    padded = jnp.pad(mixed.astype(jnp.float32), ((2, 0), (0, 0)))
    convolved = taps[0] * padded[0:row_count] + taps[1] * padded[1:row_count + 1] + taps[2] * padded[2:]
    gated = (outer_gate * convolved).astype(jnp.bfloat16)
    block_width = gated.shape[1] // N_TP
    summed = jnp.zeros((row_count, gated.shape[1]), jnp.float32)
    for block_index in range(N_TP):
        low = block_index * block_width
        partial_value = jnp.dot(gated[:, low:low + block_width], weight_output[low:low + block_width], preferred_element_type=jnp.float32).astype(jnp.bfloat16)
        partial_value = lax.optimization_barrier(partial_value)
        summed = summed + partial_value.astype(jnp.float32)
    return (stream_float + summed).astype(jnp.bfloat16)

def reference(stream, norm_gain, w_value, w_inner, w_outer, conv_taps, w_output):
    stream_now = stream
    for layer_index in range(LAYERS):
        stream_now = one_layer(stream_now, norm_gain[layer_index], w_value[layer_index], w_inner[layer_index], w_outer[layer_index], conv_taps[layer_index], w_output[layer_index])
    return stream_now
```

```python
import functools

import jax
import jax.numpy as jnp
from jax import lax
from jax.experimental import pallas as pl
from jax.experimental.pallas import tpu as pltpu
from jax.sharding import PartitionSpec as P

EPSILON = 1e-06
MESH = pl.DeviceIdType.MESH
F32 = jnp.float32
BF16 = jnp.bfloat16


def kernel(
    dims, stream, gain, w_value, w_inner, w_outer, taps, w_output, out,
    win, wout, held, normed, mix, outer, gated, tsend, s1, r1, r2a, r2b, t3a, t3b,
    r3a, r3b, tail, halo, send_sems, w_recv, swap_recv, local_sems, ag_recv, rs_recv,
):
    L, SP, TP, D, T, kb, nb, cb = dims
    Z = SP // 2
    half = T // 2
    sp, tp = lax.axis_index("sp"), lax.axis_index("tp")
    z, x = sp // 2, lax.rem(sp, 2)
    y, c = tp // 2, lax.rem(tp, 2)
    x_dev = (sp + 1 - 2 * x, tp)
    y_dev = (sp, tp + 2 - 4 * y)
    c_dev = (sp, tp + 1 - 2 * c)
    up_dev = (sp + 2, tp)
    down_dev = (sp - 2, tp)
    has_up, has_down = z < Z - 1, z > 0

    barrier = pltpu.get_barrier_semaphore()
    for dev in (x_dev, y_dev, c_dev):
        pl.semaphore_signal(barrier, inc=1, device_id=dev, device_id_type=MESH)
    for cond, dev in ((has_up, up_dev), (has_down, down_dev)):
        @pl.when(cond)
        def _(dev=dev):
            pl.semaphore_signal(barrier, inc=1, device_id=dev, device_id_type=MESH)
    peers = 3 + has_up.astype(jnp.int32) + has_down.astype(jnp.int32)
    pl.semaphore_wait(barrier, peers)

    sends = []

    def make(src, dst, recv, dev):
        slot = len(sends)
        copy = lambda: pltpu.make_async_remote_copy(
            src_ref=src(), dst_ref=dst(), send_sem=send_sems.at[slot], recv_sem=recv(),
            device_id=dev, device_id_type=MESH)
        return copy

    def send(src, dst, recv, dev):
        copy = make(lambda: src, lambda: dst, lambda: recv, dev)
        sends.append((None, copy))
        copy().start()
        return copy

    def await_recv(ref, sem, dev=x_dev):
        pltpu.make_async_remote_copy(
            src_ref=ref, dst_ref=ref, send_sem=send_sems.at[0], recv_sem=sem,
            device_id=dev, device_id_type=MESH).wait_recv()

    w_in = (w_value, w_inner, w_outer)
    col = lambda q: pl.ds(pl.multiple_of(q * nb, nb), nb)
    krow = lambda s: pl.ds(pl.multiple_of(s * kb, kb), kb)

    def parts(l, s):
        return (win.at[l, :, krow(s), :], wout.at[l, s])

    def swap_parts(l, q, s):
        for i in range(3):
            yield i, w_in[i].at[l, :, col(q)], win.at[l, i, krow(s), :]
        yield 3, w_output.at[l, col(q), :], wout.at[l, s]

    def local_copies(l):
        return [pltpu.make_async_copy(src, dst, local_sems.at[l, i])
                for i, src, dst in swap_parts(l, x, sp)]

    def swap_start(l):
        for i, src, dst in swap_parts(l, 1 - x, sp):
            send(src, dst, swap_recv.at[l, i], x_dev)

    def swap_wait(l):
        for i, src, dst in swap_parts(l, x, x_dev[0]):
            await_recv(dst, swap_recv.at[l, i])

    def relay(l, h, own):
        for sign, neighbour, dev in ((-1, has_up, up_dev), (1, has_down, down_dev)):
            origin = z + sign * h
            cond = jnp.logical_and(neighbour, jnp.logical_and(origin >= 0, origin < Z))
            picks = ((x if own else 1 - x),) if h == 0 else (0, 1)
            group = []
            for p in picks:
                for part in range(2):
                    copy = make(
                        lambda p=p, part=part, origin=origin: parts(l, 2 * origin + p)[part],
                        lambda p=p, part=part, origin=origin: parts(l, 2 * origin + p)[part],
                        lambda p=p, part=part, origin=origin: w_recv.at[l, 2 * origin + p, part],
                        dev)
                    sends.append((cond, copy))
                    group.append((p, part, copy))

            @pl.when(cond)
            def _(group=group, origin=origin, dev=dev):
                for p, part, copy in group:
                    if h > 0:
                        s = 2 * origin + p
                        await_recv(parts(l, s)[part], w_recv.at[l, s, part], dev)
                    copy().start()

    def weights_done(l, part):
        for d in range(1, Z):
            for sign, neighbour in ((-1, has_up), (1, has_down)):
                origin = z + sign * d
                inside = jnp.logical_and(origin >= 0, origin < Z)

                @pl.when(jnp.logical_and(jnp.logical_not(neighbour), inside))
                def _(origin=origin):
                    for p in range(2):
                        s = 2 * origin + p
                        await_recv(parts(l, s)[part], w_recv.at[l, s, part])

    rows_of = {0: pl.ds(0, half), 1: pl.ds(half, half)}

    def gather_start(l):
        for hf, dev in ((1, x_dev), (0, y_dev), (0, x_dev), (1, y_dev)):
            ref = held.at[l, tp, x, rows_of[hf], :]
            send(ref, ref, ag_recv.at[l, tp, x, hf], dev)
        ref = held.at[l, tp, x]
        send(ref, ref, ag_recv.at[l, tp, x, 0], c_dev)

    def gather_rest(l):
        ox, oy = 1 - x, y_dev[1]

        def got(j, xx, hf):
            await_recv(held.at[l, j, xx, rows_of[hf], :], ag_recv.at[l, j, xx, hf])

        got(tp, ox, 1)
        ref = held.at[l, tp, ox, rows_of[1], :]
        send(ref, ref, ag_recv.at[l, tp, ox, 1], y_dev)
        got(oy, x, 0)
        ref = held.at[l, oy, x, rows_of[0], :]
        send(ref, ref, ag_recv.at[l, oy, x, 0], x_dev)
        for j, xx, waits in ((tp, ox, (0,)), (oy, x, (1,)), (oy, ox, (0, 1))):
            for hf in waits:
                got(j, xx, hf)
            ref = held.at[l, j, xx]
            send(ref, ref, ag_recv.at[l, j, xx, 0], c_dev)
        cj, coy = c_dev[1], c_dev[1] + 2 - 4 * y
        for j in (cj, coy):
            for xx in range(2):
                await_recv(held.at[l, j, xx], ag_recv.at[l, j, xx, 0])

    nr = min(128, T)
    per = T // nr

    def normalize(l):
        def body(i, carry):
            xx, r = i // per, lax.rem(i, per)
            rows = pl.ds(pl.multiple_of(r * nr, nr), nr)
            blocks = [held[l, j, xx, rows, :].astype(F32) for j in range(TP)]
            total = sum(jnp.sum(b * b, axis=-1, keepdims=True) for b in blocks)
            scale = lax.rsqrt(total * (1.0 / D) + EPSILON)
            to = pl.ds(pl.multiple_of(i * nr, nr), nr)
            for j in range(TP):
                g = gain[l:l + 1, j * cb:(j + 1) * cb]
                normed[to, j * cb:(j + 1) * cb] = (blocks[j] * scale * g).astype(BF16)
            return carry
        lax.fori_loop(0, 2 * per, body, 0)

    mb = min(256, T)
    mper = T // mb

    def project(l):
        def body(i, carry):
            rows = pl.ds(pl.multiple_of(i * mb, mb), mb)
            n = normed[rows, :]
            v = jnp.dot(n, win[l, 0], preferred_element_type=F32)
            g = jnp.dot(n, win[l, 1], preferred_element_type=F32)
            mix[pl.ds(pl.multiple_of(16 + i * mb, 16), mb), :] = (g * v).astype(BF16).astype(F32)
            outer[rows, :] = jnp.dot(n, win[l, 2], preferred_element_type=F32)
            return carry
        lax.fori_loop(0, 2 * mper, body, 0)
        tail[l] = mix[2 * T:2 * T + 16, :].astype(BF16)
        copy = make(lambda: tail.at[l], lambda: halo.at[l], lambda: rs_recv.at[l, 0], up_dev)
        sends.append((has_up, copy))

        @pl.when(has_up)
        def _():
            copy().start()

    def w_block(l, j):
        per_tp = SP // TP
        return jnp.concatenate([wout[l, j * per_tp + q] for q in range(per_tp)], axis=1)

    def convolve(l):
        mix[0:16, :] = jnp.zeros((16, nb), F32)

        @pl.when(has_down)
        def _():
            await_recv(halo.at[l], rs_recv.at[l, 0])
            mix[0:16, :] = halo[l].astype(F32)

        tap = taps[l, :, col(x)]

        def body(i, carry):
            m = mix[pl.ds(pl.multiple_of(8 + i * mb, 8), mb + 8), :]
            conv = tap[0:1] * m[6:6 + mb] + tap[1:2] * m[7:7 + mb] + tap[2:3] * m[8:8 + mb]
            rows = pl.ds(pl.multiple_of(i * mb, mb), mb)
            gated[rows, :] = (outer[rows, :] * conv).astype(BF16)
            return carry
        lax.fori_loop(0, 2 * mper, body, 0)

    def outputs(l, target, core, finish):
        for yj in range(2):
            j = 2 * yj + core
            w = w_block(l, j)

            def body(i, carry):
                xx, r = i // mper, lax.rem(i, mper)
                g = gated[pl.ds(pl.multiple_of(i * mb, mb), mb), :]
                t = jnp.dot(g, w, preferred_element_type=F32).astype(BF16)
                rows = pl.ds(pl.multiple_of(r * mb, mb), mb)
                if finish:
                    t = (t.astype(F32) + r1[l, yj, xx, rows, :].astype(F32)).astype(BF16)
                target[l, yj, xx, rows, :] = t
                return carry
            if finish:
                await_recv(r1.at[l, yj], rs_recv.at[l, 1 + yj])
            lax.fori_loop(0, 2 * mper, body, 0)
            if not finish:
                send(tsend.at[l, yj], r1.at[l, yj], rs_recv.at[l, 1 + yj], c_dev)

    def f(ref):
        return ref.astype(F32)

    def reduce(l, store):
        A, B = rows_of[0], rows_of[1]
        send(s1.at[l, :, 1 - x, A, :], r2a.at[l], rs_recv.at[l, 3], x_dev)
        send(s1.at[l, 1 - y, :, B, :], r2b.at[l], rs_recv.at[l, 4], y_dev)
        await_recv(r2a.at[l], rs_recv.at[l, 3])
        t3a[l] = (f(s1[l, 1 - y, x, A, :]) + f(r2a[l, 1 - y])).astype(BF16)
        send(t3a.at[l], r3a.at[l], rs_recv.at[l, 5], y_dev)
        await_recv(r2b.at[l], rs_recv.at[l, 4])
        t3b[l] = (f(s1[l, y, 1 - x, B, :]) + f(r2b[l, 1 - x])).astype(BF16)
        send(t3b.at[l], r3b.at[l], rs_recv.at[l, 6], x_dev)
        await_recv(r3a.at[l], rs_recv.at[l, 5])
        branch = f(s1[l, y, x, A, :]) + f(r2a[l, y]) + f(r3a[l])
        store(A, (f(held[l, tp, x, A, :]) + branch).astype(BF16))
        await_recv(r3b.at[l], rs_recv.at[l, 6])
        branch = f(s1[l, y, x, B, :]) + f(r2b[l, x]) + f(r3b[l])
        store(B, (f(held[l, tp, x, B, :]) + branch).astype(BF16))

    copies = [local_copies(l) for l in range(L)]
    for group in copies:
        for copy in group:
            copy.start()
    swap_start(0)
    for copy in copies[0]:
        copy.wait()
    relay(0, 0, True)
    held[0, tp, x] = stream[...]
    gather_start(0)
    swap_wait(0)
    relay(0, 0, False)
    gather_rest(0)
    for l in range(1, L):
        swap_start(l)
    normalize(0)
    for h in range(1, Z - 1):
        relay(0, h, True)
    for l in range(L):
        if l + 1 < L:
            for copy in copies[l + 1]:
                copy.wait()
            swap_wait(l + 1)
            relay(l + 1, 0, True)
            relay(l + 1, 0, False)
        weights_done(l, 0)
        project(l)
        convolve(l)
        weights_done(l, 1)
        outputs(l, tsend, 1 - c, False)
        outputs(l, s1, c, True)
        if l + 1 < L:
            def store(rows, value, l=l):
                held[l + 1, tp, x, rows, :] = value
            reduce(l, store)
            gather_start(l + 1)
            if Z > 2:
                relay(l + 1, 1, True)
            gather_rest(l + 1)
            normalize(l + 1)
            for h in range(2, Z - 1):
                relay(l + 1, h, True)
        else:
            def store(rows, value):
                out[rows, :] = value
            reduce(l, store)

    for cond, copy in sends:
        if cond is None:
            copy().wait_send()
        else:
            @pl.when(cond)
            def _(copy=copy):
                copy().wait_send()


def on_device(SP, TP, stream, norm_gain, w_value, w_inner, w_outer, conv_taps, w_output):
    L, kb, cb = w_value.shape
    T, D = stream.shape[0], norm_gain.shape[1]
    nb, Z = cb // 2, SP // 2
    dims = (L, SP, TP, D, T, kb, nb, cb)
    vmem = pl.BlockSpec(memory_space=pltpu.VMEM)
    hbm = pl.BlockSpec(memory_space=pl.ANY)
    half = T // 2
    n_sends = L * (4 + 4 * (1 + 2 * max(Z - 2, 0)) * 2 + 16 + 8)
    return pl.pallas_call(
        functools.partial(kernel, dims),
        out_shape=jax.ShapeDtypeStruct((T, cb), BF16),
        in_specs=[vmem, vmem, hbm, hbm, hbm, vmem, hbm],
        out_specs=vmem,
        scratch_shapes=[
            pltpu.VMEM((L, 3, D, nb), BF16),
            pltpu.VMEM((L, SP, nb, kb), BF16),
            pltpu.VMEM((L, TP, 2, T, cb), BF16),
            pltpu.VMEM((2 * T, D), BF16),
            pltpu.VMEM((2 * T + 16, nb), F32),
            pltpu.VMEM((2 * T, nb), F32),
            pltpu.VMEM((2 * T, nb), BF16),
            pltpu.VMEM((L, 2, 2, T, cb), BF16),
            pltpu.VMEM((L, 2, 2, T, cb), BF16),
            pltpu.VMEM((L, 2, 2, T, cb), BF16),
            pltpu.VMEM((L, 2, half, cb), BF16),
            pltpu.VMEM((L, 2, half, cb), BF16),
            pltpu.VMEM((L, half, cb), BF16),
            pltpu.VMEM((L, half, cb), BF16),
            pltpu.VMEM((L, half, cb), BF16),
            pltpu.VMEM((L, half, cb), BF16),
            pltpu.VMEM((L, 16, nb), BF16),
            pltpu.VMEM((L, 16, nb), BF16),
            pltpu.SemaphoreType.DMA((n_sends,)),
            pltpu.SemaphoreType.DMA((L, SP, 2)),
            pltpu.SemaphoreType.DMA((L, 4)),
            pltpu.SemaphoreType.DMA((L, 4)),
            pltpu.SemaphoreType.DMA((L, TP, 2, 2)),
            pltpu.SemaphoreType.DMA((L, 7)),
        ],
        compiler_params=pltpu.CompilerParams(
            collective_id=0, has_side_effects=True, vmem_limit_bytes=60 * 1024 * 1024
        ),
    )(stream, norm_gain, w_value, w_inner, w_outer, conv_taps, w_output)


def solution(mesh):
    SP, TP = mesh.shape["sp"], mesh.shape["tp"]
    in_specs = (
        P("sp", "tp"),
        P(),
        P(None, "sp", "tp"),
        P(None, "sp", "tp"),
        P(None, "sp", "tp"),
        P(None, None, "tp"),
        P(None, "tp", "sp"),
    )
    return jax.shard_map(
        functools.partial(on_device, SP, TP),
        mesh=mesh, in_specs=in_specs, out_specs=P("sp", "tp"), check_vma=False,
    )
```

```python
import functools

import jax
import jax.numpy as jnp
from jax import lax
from jax.experimental import pallas as pl
from jax.experimental.pallas import tpu as pltpu
from jax.sharding import PartitionSpec as P

EPSILON = 1e-06
MESH = pl.DeviceIdType.MESH
F32 = jnp.float32
BF16 = jnp.bfloat16


def kernel(
    dims, stream, gain, w_value, w_inner, w_outer, taps, w_output, out,
    win, wout, held, normed, mix, outer, gated, tsend, s1, r1, r2a, r2b, t3a, t3b,
    r3a, r3b, tail, halo, send_sems, w_recv, swap_recv, local_sems, ag_recv, rs_recv,
):
    L, SP, TP, D, T, kb, nb, cb = dims
    Z = SP // 2
    half = T // 2
    sp, tp = lax.axis_index("sp"), lax.axis_index("tp")
    z, x = sp // 2, lax.rem(sp, 2)
    y, c = tp // 2, lax.rem(tp, 2)
    x_dev = (sp + 1 - 2 * x, tp)
    y_dev = (sp, tp + 2 - 4 * y)
    c_dev = (sp, tp + 1 - 2 * c)
    up_dev = (sp + 2, tp)
    down_dev = (sp - 2, tp)
    has_up, has_down = z < Z - 1, z > 0

    barrier = pltpu.get_barrier_semaphore()
    for dev in (x_dev, y_dev, c_dev):
        pl.semaphore_signal(barrier, inc=1, device_id=dev, device_id_type=MESH)
    for cond, dev in ((has_up, up_dev), (has_down, down_dev)):
        @pl.when(cond)
        def _(dev=dev):
            pl.semaphore_signal(barrier, inc=1, device_id=dev, device_id_type=MESH)
    peers = 3 + has_up.astype(jnp.int32) + has_down.astype(jnp.int32)
    pl.semaphore_wait(barrier, peers)

    sends = []

    def make(src, dst, recv, dev):
        slot = len(sends)
        copy = lambda: pltpu.make_async_remote_copy(
            src_ref=src(), dst_ref=dst(), send_sem=send_sems.at[slot], recv_sem=recv(),
            device_id=dev, device_id_type=MESH)
        return copy

    def send(src, dst, recv, dev):
        copy = make(lambda: src, lambda: dst, lambda: recv, dev)
        sends.append((None, copy))
        copy().start()
        return copy

    def await_recv(ref, sem, dev=x_dev):
        pltpu.make_async_remote_copy(
            src_ref=ref, dst_ref=ref, send_sem=send_sems.at[0], recv_sem=sem,
            device_id=dev, device_id_type=MESH).wait_recv()

    w_in = (w_value, w_inner, w_outer)
    col = lambda q: pl.ds(pl.multiple_of(q * nb, nb), nb)
    krow = lambda s: pl.ds(pl.multiple_of(s * kb, kb), kb)

    def parts(l, s):
        return (win.at[l, :, krow(s), :], wout.at[l, s])

    def swap_parts(l, q, s):
        for i in range(3):
            yield i, w_in[i].at[l, :, col(q)], win.at[l, i, krow(s), :]
        yield 3, w_output.at[l, col(q), :], wout.at[l, s]

    def local_copies(l):
        return [pltpu.make_async_copy(src, dst, local_sems.at[l, i])
                for i, src, dst in swap_parts(l, x, sp)]

    def swap_start(l):
        for i, src, dst in swap_parts(l, 1 - x, sp):
            send(src, dst, swap_recv.at[l, i], x_dev)

    def swap_wait(l):
        for i, src, dst in swap_parts(l, x, x_dev[0]):
            await_recv(dst, swap_recv.at[l, i])

    middle = jnp.logical_and(has_up, has_down)
    ends = jnp.logical_not(middle)
    IN, OUT = 0, 1

    def relay(l, part, h, picks=None, only=None):
        for sign, neighbour, dev in ((-1, has_up, up_dev), (1, has_down, down_dev)):
            origin = z + sign * h
            cond = jnp.logical_and(neighbour, jnp.logical_and(origin >= 0, origin < Z))
            if only is not None:
                cond = jnp.logical_and(cond, only)
            group = []
            for p in (picks or (x, 1 - x)):
                s = 2 * origin + p

                def copy(s=s, dev=dev, slot=len(sends)):
                    ref = parts(l, s)[part]
                    return pltpu.make_async_remote_copy(
                        src_ref=ref, dst_ref=ref, send_sem=send_sems.at[slot],
                        recv_sem=w_recv.at[l, s, part], device_id=dev, device_id_type=MESH)
                sends.append((cond, copy))
                group.append((s, copy))

            @pl.when(cond)
            def _(group=group, dev=dev):
                for s, copy in group:
                    if h > 0:
                        await_recv(parts(l, s)[part], w_recv.at[l, s, part], dev)
                    copy().start()

    def weights_done(l, part):
        for d in range(1, Z):
            for sign, neighbour in ((-1, has_up), (1, has_down)):
                origin = z + sign * d
                inside = jnp.logical_and(origin >= 0, origin < Z)

                @pl.when(jnp.logical_and(jnp.logical_not(neighbour), inside))
                def _(origin=origin):
                    for p in range(2):
                        s = 2 * origin + p
                        await_recv(parts(l, s)[part], w_recv.at[l, s, part])

    rows_of = {0: pl.ds(0, half), 1: pl.ds(half, half)}

    def gather_start(l):
        for hf, dev in ((1, x_dev), (0, y_dev), (0, x_dev), (1, y_dev)):
            ref = held.at[l, tp, x, rows_of[hf], :]
            send(ref, ref, ag_recv.at[l, tp, x, hf], dev)
        ref = held.at[l, tp, x]
        send(ref, ref, ag_recv.at[l, tp, x, 0], c_dev)

    def gather_rest(l):
        ox, oy = 1 - x, y_dev[1]

        def got(j, xx, hf):
            await_recv(held.at[l, j, xx, rows_of[hf], :], ag_recv.at[l, j, xx, hf])

        got(tp, ox, 1)
        ref = held.at[l, tp, ox, rows_of[1], :]
        send(ref, ref, ag_recv.at[l, tp, ox, 1], y_dev)
        got(oy, x, 0)
        ref = held.at[l, oy, x, rows_of[0], :]
        send(ref, ref, ag_recv.at[l, oy, x, 0], x_dev)
        for j, xx, waits in ((tp, ox, (0,)), (oy, x, (1,)), (oy, ox, (0, 1))):
            for hf in waits:
                got(j, xx, hf)
            ref = held.at[l, j, xx]
            send(ref, ref, ag_recv.at[l, j, xx, 0], c_dev)
        cj, coy = c_dev[1], c_dev[1] + 2 - 4 * y
        for j in (cj, coy):
            for xx in range(2):
                await_recv(held.at[l, j, xx], ag_recv.at[l, j, xx, 0])

    nr = min(128, T)
    per = T // nr

    def normalize(l):
        def body(i, carry):
            xx, r = i // per, lax.rem(i, per)
            rows = pl.ds(pl.multiple_of(r * nr, nr), nr)
            blocks = [held[l, j, xx, rows, :].astype(F32) for j in range(TP)]
            total = sum(jnp.sum(b * b, axis=-1, keepdims=True) for b in blocks)
            scale = lax.rsqrt(total * (1.0 / D) + EPSILON)
            to = pl.ds(pl.multiple_of(i * nr, nr), nr)
            for j in range(TP):
                g = gain[l:l + 1, j * cb:(j + 1) * cb]
                normed[to, j * cb:(j + 1) * cb] = (blocks[j] * scale * g).astype(BF16)
            return carry
        lax.fori_loop(0, 2 * per, body, 0)

    mb = min(256, T)
    mper = T // mb

    def project(l):
        def body(i, carry):
            rows = pl.ds(pl.multiple_of(i * mb, mb), mb)
            n = normed[rows, :]
            v = jnp.dot(n, win[l, 0], preferred_element_type=F32)
            g = jnp.dot(n, win[l, 1], preferred_element_type=F32)
            mix[pl.ds(pl.multiple_of(16 + i * mb, 16), mb), :] = (g * v).astype(BF16).astype(F32)
            outer[rows, :] = jnp.dot(n, win[l, 2], preferred_element_type=F32)
            return carry
        lax.fori_loop(0, 2 * mper, body, 0)
        tail[l] = mix[2 * T:2 * T + 16, :].astype(BF16)
        copy = make(lambda: tail.at[l], lambda: halo.at[l], lambda: rs_recv.at[l, 0], up_dev)
        sends.append((has_up, copy))

        @pl.when(has_up)
        def _():
            copy().start()

    def w_block(l, j):
        per_tp = SP // TP
        return jnp.concatenate([wout[l, j * per_tp + q] for q in range(per_tp)], axis=1)

    def convolve(l):
        mix[0:16, :] = jnp.zeros((16, nb), F32)

        @pl.when(has_down)
        def _():
            await_recv(halo.at[l], rs_recv.at[l, 0])
            mix[0:16, :] = halo[l].astype(F32)

        tap = taps[l, :, col(x)]

        def body(i, carry):
            m = mix[pl.ds(pl.multiple_of(8 + i * mb, 8), mb + 8), :]
            conv = tap[0:1] * m[6:6 + mb] + tap[1:2] * m[7:7 + mb] + tap[2:3] * m[8:8 + mb]
            rows = pl.ds(pl.multiple_of(i * mb, mb), mb)
            gated[rows, :] = (outer[rows, :] * conv).astype(BF16)
            return carry
        lax.fori_loop(0, 2 * mper, body, 0)

    def outputs(l, target, core, finish):
        for yj in range(2):
            j = 2 * yj + core
            w = w_block(l, j)

            def body(i, carry):
                xx, r = i // mper, lax.rem(i, mper)
                g = gated[pl.ds(pl.multiple_of(i * mb, mb), mb), :]
                t = jnp.dot(g, w, preferred_element_type=F32).astype(BF16)
                rows = pl.ds(pl.multiple_of(r * mb, mb), mb)
                if finish:
                    t = (t.astype(F32) + r1[l, yj, xx, rows, :].astype(F32)).astype(BF16)
                target[l, yj, xx, rows, :] = t
                return carry
            if finish:
                await_recv(r1.at[l, yj], rs_recv.at[l, 1 + yj])
            lax.fori_loop(0, 2 * mper, body, 0)
            if not finish:
                send(tsend.at[l, yj], r1.at[l, yj], rs_recv.at[l, 1 + yj], c_dev)

    def f(ref):
        return ref.astype(F32)

    def reduce(l, store):
        A, B = rows_of[0], rows_of[1]
        send(s1.at[l, :, 1 - x, A, :], r2a.at[l], rs_recv.at[l, 3], x_dev)
        send(s1.at[l, 1 - y, :, B, :], r2b.at[l], rs_recv.at[l, 4], y_dev)
        await_recv(r2a.at[l], rs_recv.at[l, 3])
        t3a[l] = (f(s1[l, 1 - y, x, A, :]) + f(r2a[l, 1 - y])).astype(BF16)
        send(t3a.at[l], r3a.at[l], rs_recv.at[l, 5], y_dev)
        await_recv(r2b.at[l], rs_recv.at[l, 4])
        t3b[l] = (f(s1[l, y, 1 - x, B, :]) + f(r2b[l, 1 - x])).astype(BF16)
        send(t3b.at[l], r3b.at[l], rs_recv.at[l, 6], x_dev)
        await_recv(r3a.at[l], rs_recv.at[l, 5])
        branch = f(s1[l, y, x, A, :]) + f(r2a[l, y]) + f(r3a[l])
        store(A, (f(held[l, tp, x, A, :]) + branch).astype(BF16))
        await_recv(r3b.at[l], rs_recv.at[l, 6])
        branch = f(s1[l, y, x, B, :]) + f(r2b[l, x]) + f(r3b[l])
        store(B, (f(held[l, tp, x, B, :]) + branch).astype(BF16))

    copies = [local_copies(l) for l in range(L)]
    for group in copies:
        for copy in group:
            copy.start()
    swap_start(0)
    for copy in copies[0]:
        copy.wait()
    relay(0, IN, 0, (x,))
    held[0, tp, x] = stream[...]
    gather_start(0)
    swap_wait(0)
    relay(0, IN, 0, (1 - x,))
    relay(0, OUT, 0, only=ends)
    if Z > 2:
        relay(0, IN, 1)
    gather_rest(0)
    for l in range(1, L):
        swap_start(l)
    for h in range(2, Z - 1):
        relay(0, IN, h)
    relay(0, OUT, 0, only=middle)
    normalize(0)
    for l in range(1, L):
        for copy in copies[l]:
            copy.wait()
        swap_wait(l)
        relay(l, IN, 0, only=ends)
        relay(l, OUT, 0, only=ends)
    for l in range(L):
        weights_done(l, IN)
        project(l)
        if l + 1 < L:
            for h in range(1, Z - 1):
                relay(l, OUT, h)
            relay(l + 1, IN, 0, only=middle)
        convolve(l)
        weights_done(l, OUT)
        outputs(l, tsend, 1 - c, False)
        outputs(l, s1, c, True)
        if l + 1 < L:
            def store(rows, value, l=l):
                held[l + 1, tp, x, rows, :] = value
            if Z > 2:
                relay(l + 1, IN, 1)
            reduce(l, store)
            gather_start(l + 1)
            for h in range(2, Z - 1):
                relay(l + 1, IN, h)
            gather_rest(l + 1)
            relay(l + 1, OUT, 0, only=middle)
            normalize(l + 1)
            if l + 2 == L:
                for h in range(1, Z - 1):
                    relay(l + 1, OUT, h)
        else:
            def store(rows, value):
                out[rows, :] = value
            reduce(l, store)

    for cond, copy in sends:
        if cond is None:
            copy().wait_send()
        else:
            @pl.when(cond)
            def _(copy=copy):
                copy().wait_send()


def on_device(SP, TP, stream, norm_gain, w_value, w_inner, w_outer, conv_taps, w_output):
    L, kb, cb = w_value.shape
    T, D = stream.shape[0], norm_gain.shape[1]
    nb, Z = cb // 2, SP // 2
    dims = (L, SP, TP, D, T, kb, nb, cb)
    vmem = pl.BlockSpec(memory_space=pltpu.VMEM)
    hbm = pl.BlockSpec(memory_space=pl.ANY)
    half = T // 2
    n_sends = L * (4 + 8 * max(Z - 1, 1) + 8 + 9 + 8)
    return pl.pallas_call(
        functools.partial(kernel, dims),
        out_shape=jax.ShapeDtypeStruct((T, cb), BF16),
        in_specs=[vmem, vmem, hbm, hbm, hbm, vmem, hbm],
        out_specs=vmem,
        scratch_shapes=[
            pltpu.VMEM((L, 3, D, nb), BF16),
            pltpu.VMEM((L, SP, nb, kb), BF16),
            pltpu.VMEM((L, TP, 2, T, cb), BF16),
            pltpu.VMEM((2 * T, D), BF16),
            pltpu.VMEM((2 * T + 16, nb), F32),
            pltpu.VMEM((2 * T, nb), F32),
            pltpu.VMEM((2 * T, nb), BF16),
            pltpu.VMEM((L, 2, 2, T, cb), BF16),
            pltpu.VMEM((L, 2, 2, T, cb), BF16),
            pltpu.VMEM((L, 2, 2, T, cb), BF16),
            pltpu.VMEM((L, 2, half, cb), BF16),
            pltpu.VMEM((L, 2, half, cb), BF16),
            pltpu.VMEM((L, half, cb), BF16),
            pltpu.VMEM((L, half, cb), BF16),
            pltpu.VMEM((L, half, cb), BF16),
            pltpu.VMEM((L, half, cb), BF16),
            pltpu.VMEM((L, 16, nb), BF16),
            pltpu.VMEM((L, 16, nb), BF16),
            pltpu.SemaphoreType.DMA((n_sends,)),
            pltpu.SemaphoreType.DMA((L, SP, 2)),
            pltpu.SemaphoreType.DMA((L, 4)),
            pltpu.SemaphoreType.DMA((L, 4)),
            pltpu.SemaphoreType.DMA((L, TP, 2, 2)),
            pltpu.SemaphoreType.DMA((L, 7)),
        ],
        compiler_params=pltpu.CompilerParams(
            collective_id=0, has_side_effects=True, vmem_limit_bytes=60 * 1024 * 1024
        ),
    )(stream, norm_gain, w_value, w_inner, w_outer, conv_taps, w_output)


def solution(mesh):
    SP, TP = mesh.shape["sp"], mesh.shape["tp"]
    in_specs = (
        P("sp", "tp"),
        P(),
        P(None, "sp", "tp"),
        P(None, "sp", "tp"),
        P(None, "sp", "tp"),
        P(None, None, "tp"),
        P(None, "tp", "sp"),
    )
    return jax.shard_map(
        functools.partial(on_device, SP, TP),
        mesh=mesh, in_specs=in_specs, out_specs=P("sp", "tp"), check_vma=False,
    )
```

```python
import functools

import jax
import jax.numpy as jnp
from jax import lax
from jax.experimental import pallas as pl
from jax.experimental.pallas import tpu as pltpu
from jax.sharding import PartitionSpec as P

EPSILON = 1e-06
MESH = pl.DeviceIdType.MESH
F32 = jnp.float32
BF16 = jnp.bfloat16


def kernel(
    dims, stream, gain, w_value, w_inner, w_outer, taps, w_output, out,
    win, wout, held, normed, mix, outer, gated, tsend, s1, r1, r2a, r2b, t3a, t3b,
    r3a, r3b, tail, halo, send_sems, w_recv, swap_recv, local_sems, ag_recv, rs_recv,
):
    L, SP, TP, D, T, kb, nb, cb = dims
    Z = SP // 2
    half = T // 2
    sp, tp = lax.axis_index("sp"), lax.axis_index("tp")
    z, x = sp // 2, lax.rem(sp, 2)
    y, c = tp // 2, lax.rem(tp, 2)
    x_dev = (sp + 1 - 2 * x, tp)
    y_dev = (sp, tp + 2 - 4 * y)
    c_dev = (sp, tp + 1 - 2 * c)
    up_dev = (sp + 2, tp)
    down_dev = (sp - 2, tp)
    has_up, has_down = z < Z - 1, z > 0

    first = (2 * z >= Z).astype(jnp.int32)
    sends = []

    def make(src, dst, recv, dev):
        slot = len(sends)
        copy = lambda: pltpu.make_async_remote_copy(
            src_ref=src(), dst_ref=dst(), send_sem=send_sems.at[slot], recv_sem=recv(),
            device_id=dev, device_id_type=MESH)
        return copy

    def send(src, dst, recv, dev):
        copy = make(lambda: src, lambda: dst, lambda: recv, dev)
        sends.append((None, copy))
        copy().start()
        return copy

    def await_recv(ref, sem, dev=x_dev):
        pltpu.make_async_remote_copy(
            src_ref=ref, dst_ref=ref, send_sem=send_sems.at[0], recv_sem=sem,
            device_id=dev, device_id_type=MESH).wait_recv()

    w_in = (w_value, w_inner, w_outer)
    col = lambda q: pl.ds(pl.multiple_of(q * nb, nb), nb)
    krow = lambda s: pl.ds(pl.multiple_of(s * kb, kb), kb)

    def parts(l, s):
        return (win.at[l, :, krow(s), :], wout.at[l, s])

    def swap_parts(l, q, s):
        for i in range(3):
            yield i, w_in[i].at[l, :, col(q)], win.at[l, i, krow(s), :]
        yield 3, w_output.at[l, col(q), :], wout.at[l, s]

    def local_copies(l):
        return [pltpu.make_async_copy(src, dst, local_sems.at[l, i])
                for i, src, dst in swap_parts(l, x, sp)]

    def swap_start(l):
        for i, src, dst in swap_parts(l, 1 - x, sp):
            send(src, dst, swap_recv.at[l, i], x_dev)

    def swap_wait(l, part):
        for i, src, dst in swap_parts(l, x, x_dev[0]):
            if (i == 3) == (part == OUT):
                await_recv(dst, swap_recv.at[l, i])

    middle = jnp.logical_and(has_up, has_down)
    ends = jnp.logical_not(middle)
    IN, OUT = 0, 1

    def relay(l, part, h, picks=None, only=None):
        for p in (picks or (x, 1 - x)):
            for sign, neighbour, dev in ((-1, has_up, up_dev), (1, has_down, down_dev)):
                origin = z + sign * h
                cond = jnp.logical_and(neighbour, jnp.logical_and(origin >= 0, origin < Z))
                if only is not None:
                    cond = jnp.logical_and(cond, only)
                s = 2 * origin + p

                def copy(s=s, dev=dev, slot=len(sends)):
                    ref = parts(l, s)[part]
                    return pltpu.make_async_remote_copy(
                        src_ref=ref, dst_ref=ref, send_sem=send_sems.at[slot],
                        recv_sem=w_recv.at[l, s, part], device_id=dev, device_id_type=MESH)
                sends.append((cond, copy))

                @pl.when(cond)
                def _(s=s, copy=copy, dev=dev):
                    if h > 0:
                        await_recv(parts(l, s)[part], w_recv.at[l, s, part], dev)
                    copy().start()

    def weights_done(l, part, near=None):
        for d in range(1, Z):
            for sign, neighbour in ((-1, has_up), (1, has_down)):
                origin = z + sign * d
                inside = jnp.logical_and(origin >= 0, origin < Z)
                if near is not None:
                    same = (2 * origin >= Z) == (first == 1)
                    inside = jnp.logical_and(inside, same if near else jnp.logical_not(same))

                @pl.when(jnp.logical_and(jnp.logical_not(neighbour), inside))
                def _(origin=origin):
                    for p in range(2):
                        s = 2 * origin + p
                        await_recv(parts(l, s)[part], w_recv.at[l, s, part])

    rows_of = {0: pl.ds(0, half), 1: pl.ds(half, half)}

    def gather_start(l):
        for hf, dev in ((1, x_dev), (0, y_dev), (0, x_dev), (1, y_dev)):
            ref = held.at[l, tp, x, rows_of[hf], :]
            send(ref, ref, ag_recv.at[l, tp, x, hf], dev)
        ref = held.at[l, tp, x]
        send(ref, ref, ag_recv.at[l, tp, x, 0], c_dev)

    def gather_rest(l):
        ox, oy = 1 - x, y_dev[1]

        def got(j, xx, hf):
            await_recv(held.at[l, j, xx, rows_of[hf], :], ag_recv.at[l, j, xx, hf])

        got(tp, ox, 1)
        ref = held.at[l, tp, ox, rows_of[1], :]
        send(ref, ref, ag_recv.at[l, tp, ox, 1], y_dev)
        got(oy, x, 0)
        ref = held.at[l, oy, x, rows_of[0], :]
        send(ref, ref, ag_recv.at[l, oy, x, 0], x_dev)
        for j, xx, waits in ((tp, ox, (0,)), (oy, x, (1,)), (oy, ox, (0, 1))):
            for hf in waits:
                got(j, xx, hf)
            ref = held.at[l, j, xx]
            send(ref, ref, ag_recv.at[l, j, xx, 0], c_dev)
        cj, coy = c_dev[1], c_dev[1] + 2 - 4 * y
        for j in (cj, coy):
            for xx in range(2):
                await_recv(held.at[l, j, xx], ag_recv.at[l, j, xx, 0])

    nr = min(128, T)
    per = T // nr

    def normalize(l):
        def body(i, carry):
            xx, r = i // per, lax.rem(i, per)
            rows = pl.ds(pl.multiple_of(r * nr, nr), nr)
            blocks = [held[l, j, xx, rows, :].astype(F32) for j in range(TP)]
            total = sum(jnp.sum(b * b, axis=-1, keepdims=True) for b in blocks)
            scale = lax.rsqrt(total * (1.0 / D) + EPSILON)
            to = pl.ds(pl.multiple_of(i * nr, nr), nr)
            for j in range(TP):
                g = gain[l:l + 1, j * cb:(j + 1) * cb]
                normed[to, j * cb:(j + 1) * cb] = (blocks[j] * scale * g).astype(BF16)
            return carry
        lax.fori_loop(0, 2 * per, body, 0)

    mb = min(256, T)
    mper = T // mb

    def project(l):
        def body(i, carry):
            rows = pl.ds(pl.multiple_of(i * mb, mb), mb)
            n = normed[rows, :]
            v = jnp.dot(n, win[l, 0], preferred_element_type=F32)
            g = jnp.dot(n, win[l, 1], preferred_element_type=F32)
            mix[pl.ds(pl.multiple_of(16 + i * mb, 16), mb), :] = (g * v).astype(BF16).astype(F32)
            outer[rows, :] = jnp.dot(n, win[l, 2], preferred_element_type=F32)
            return carry
        lax.fori_loop(0, 2 * mper, body, 0)
        tail[l] = mix[2 * T:2 * T + 16, :].astype(BF16)
        copy = make(lambda: tail.at[l], lambda: halo.at[l], lambda: rs_recv.at[l, 0], up_dev)
        sends.append((has_up, copy))

        @pl.when(has_up)
        def _():
            copy().start()

    def w_block(l, j):
        per_tp = SP // TP
        return jnp.concatenate([wout[l, j * per_tp + q] for q in range(per_tp)], axis=1)

    def convolve(l):
        mix[0:16, :] = jnp.zeros((16, nb), F32)

        @pl.when(has_down)
        def _():
            await_recv(halo.at[l], rs_recv.at[l, 0])
            mix[0:16, :] = halo[l].astype(F32)

        tap = taps[l, :, col(x)]

        def body(i, carry):
            m = mix[pl.ds(pl.multiple_of(8 + i * mb, 8), mb + 8), :]
            conv = tap[0:1] * m[6:6 + mb] + tap[1:2] * m[7:7 + mb] + tap[2:3] * m[8:8 + mb]
            rows = pl.ds(pl.multiple_of(i * mb, mb), mb)
            gated[rows, :] = (outer[rows, :] * conv).astype(BF16)
            return carry
        lax.fori_loop(0, 2 * mper, body, 0)

    def outputs(l, yj, target, core, finish):
        w = w_block(l, 2 * yj + core)

        def body(i, carry):
            xx, r = i // mper, lax.rem(i, mper)
            g = gated[pl.ds(pl.multiple_of(i * mb, mb), mb), :]
            t = jnp.dot(g, w, preferred_element_type=F32).astype(BF16)
            rows = pl.ds(pl.multiple_of(r * mb, mb), mb)
            if finish:
                t = (t.astype(F32) + r1[l, yj, xx, rows, :].astype(F32)).astype(BF16)
            target[l, yj, xx, rows, :] = t
            return carry
        if finish:
            await_recv(r1.at[l, yj], rs_recv.at[l, 1 + yj])
        lax.fori_loop(0, 2 * mper, body, 0)
        if not finish:
            send(tsend.at[l, yj], r1.at[l, yj], rs_recv.at[l, 1 + yj], c_dev)

    def output_group(l, yj):
        A, B = rows_of[0], rows_of[1]
        outputs(l, yj, tsend, 1 - c, False)
        outputs(l, yj, s1, c, True)
        send(s1.at[l, yj, 1 - x, A, :], r2a.at[l, yj], rs_recv.at[l, 3 + yj], x_dev)
        other = yj != y
        for xj in (1 - x, x):
            copy = make(
                lambda xj=xj: s1.at[l, yj, xj, B, :], lambda xj=xj: r2b.at[l, xj],
                lambda xj=xj: rs_recv.at[l, 5 + xj], y_dev)
            sends.append((other, copy))

            @pl.when(other)
            def _(copy=copy):
                copy().start()

    def f(ref):
        return ref.astype(F32)

    def reduce(l, store):
        A, B = rows_of[0], rows_of[1]
        await_recv(r2a.at[l, 1 - y], rs_recv.at[l, 4 - y])
        t3a[l] = (f(s1[l, 1 - y, x, A, :]) + f(r2a[l, 1 - y])).astype(BF16)
        send(t3a.at[l], r3a.at[l], rs_recv.at[l, 7], y_dev)
        await_recv(r2b.at[l, 1 - x], rs_recv.at[l, 6 - x])
        t3b[l] = (f(s1[l, y, 1 - x, B, :]) + f(r2b[l, 1 - x])).astype(BF16)
        send(t3b.at[l], r3b.at[l], rs_recv.at[l, 8], x_dev)
        await_recv(r2a.at[l, y], rs_recv.at[l, 3 + y])
        await_recv(r3a.at[l], rs_recv.at[l, 7])
        branch = f(s1[l, y, x, A, :]) + f(r2a[l, y]) + f(r3a[l])
        store(A, (f(held[l, tp, x, A, :]) + branch).astype(BF16))
        await_recv(r2b.at[l, x], rs_recv.at[l, 5 + x])
        await_recv(r3b.at[l], rs_recv.at[l, 8])
        branch = f(s1[l, y, x, B, :]) + f(r2b[l, x]) + f(r3b[l])
        store(B, (f(held[l, tp, x, B, :]) + branch).astype(BF16))

    copies = [local_copies(l) for l in range(L)]
    for group in copies:
        for copy in group:
            copy.start()
    held[0, tp, x] = stream[...]

    barrier = pltpu.get_barrier_semaphore()
    for dev in (x_dev, y_dev, c_dev):
        pl.semaphore_signal(barrier, inc=1, device_id=dev, device_id_type=MESH)
    for cond, dev in ((has_up, up_dev), (has_down, down_dev)):
        @pl.when(cond)
        def _(dev=dev):
            pl.semaphore_signal(barrier, inc=1, device_id=dev, device_id_type=MESH)
    peers = 3 + has_up.astype(jnp.int32) + has_down.astype(jnp.int32)
    pl.semaphore_wait(barrier, peers)

    swap_start(0)
    for copy in copies[0][:3]:
        copy.wait()
    relay(0, IN, 0, (x,))
    copies[0][3].wait()
    relay(0, OUT, 0, (x,))
    gather_start(0)
    swap_wait(0, IN)
    relay(0, IN, 0, (1 - x,))
    swap_wait(0, OUT)
    relay(0, OUT, 0, (1 - x,), only=ends)
    if Z > 2:
        relay(0, IN, 1)
    gather_rest(0)
    for l in range(1, L):
        swap_start(l)
    for h in range(2, Z - 1):
        relay(0, IN, h)
    relay(0, OUT, 0, (1 - x,), only=middle)
    normalize(0)
    for l in range(1, L):
        for copy in copies[l]:
            copy.wait()
        swap_wait(l, IN)
        swap_wait(l, OUT)
        relay(l, IN, 0, only=ends)
        relay(l, OUT, 0, only=ends)
    for l in range(L):
        weights_done(l, IN)
        project(l)
        if l + 1 < L:
            for h in range(1, Z - 1):
                relay(l, OUT, h)
            relay(l + 1, IN, 0, only=middle)
        convolve(l)
        weights_done(l, OUT, True)
        output_group(l, first)
        weights_done(l, OUT, False)
        output_group(l, 1 - first)
        if l + 1 < L:
            def store(rows, value, l=l):
                held[l + 1, tp, x, rows, :] = value
            if Z > 2:
                relay(l + 1, IN, 1)
            reduce(l, store)
            gather_start(l + 1)
            for h in range(2, Z - 1):
                relay(l + 1, IN, h)
            gather_rest(l + 1)
            relay(l + 1, OUT, 0, only=middle)
            normalize(l + 1)
            if l + 2 == L:
                for h in range(1, Z - 1):
                    relay(l + 1, OUT, h)
        else:
            def store(rows, value):
                out[rows, :] = value
            reduce(l, store)

    for cond, copy in sends:
        if cond is None:
            copy().wait_send()
        else:
            @pl.when(cond)
            def _(copy=copy):
                copy().wait_send()


def on_device(SP, TP, stream, norm_gain, w_value, w_inner, w_outer, conv_taps, w_output):
    L, kb, cb = w_value.shape
    T, D = stream.shape[0], norm_gain.shape[1]
    nb, Z = cb // 2, SP // 2
    dims = (L, SP, TP, D, T, kb, nb, cb)
    vmem = pl.BlockSpec(memory_space=pltpu.VMEM)
    hbm = pl.BlockSpec(memory_space=pl.ANY)
    half = T // 2
    n_sends = L * (4 + 8 * max(Z - 1, 1) + 8 + 10 + 13)
    return pl.pallas_call(
        functools.partial(kernel, dims),
        out_shape=jax.ShapeDtypeStruct((T, cb), BF16),
        in_specs=[vmem, vmem, hbm, hbm, hbm, vmem, hbm],
        out_specs=vmem,
        scratch_shapes=[
            pltpu.VMEM((L, 3, D, nb), BF16),
            pltpu.VMEM((L, SP, nb, kb), BF16),
            pltpu.VMEM((L, TP, 2, T, cb), BF16),
            pltpu.VMEM((2 * T, D), BF16),
            pltpu.VMEM((2 * T + 16, nb), F32),
            pltpu.VMEM((2 * T, nb), F32),
            pltpu.VMEM((2 * T, nb), BF16),
            pltpu.VMEM((L, 2, 2, T, cb), BF16),
            pltpu.VMEM((L, 2, 2, T, cb), BF16),
            pltpu.VMEM((L, 2, 2, T, cb), BF16),
            pltpu.VMEM((L, 2, half, cb), BF16),
            pltpu.VMEM((L, 2, half, cb), BF16),
            pltpu.VMEM((L, half, cb), BF16),
            pltpu.VMEM((L, half, cb), BF16),
            pltpu.VMEM((L, half, cb), BF16),
            pltpu.VMEM((L, half, cb), BF16),
            pltpu.VMEM((L, 16, nb), BF16),
            pltpu.VMEM((L, 16, nb), BF16),
            pltpu.SemaphoreType.DMA((n_sends,)),
            pltpu.SemaphoreType.DMA((L, SP, 2)),
            pltpu.SemaphoreType.DMA((L, 4)),
            pltpu.SemaphoreType.DMA((L, 4)),
            pltpu.SemaphoreType.DMA((L, TP, 2, 2)),
            pltpu.SemaphoreType.DMA((L, 9)),
        ],
        compiler_params=pltpu.CompilerParams(
            collective_id=0, has_side_effects=True, vmem_limit_bytes=60 * 1024 * 1024
        ),
    )(stream, norm_gain, w_value, w_inner, w_outer, conv_taps, w_output)


def solution(mesh):
    SP, TP = mesh.shape["sp"], mesh.shape["tp"]
    in_specs = (
        P("sp", "tp"),
        P(),
        P(None, "sp", "tp"),
        P(None, "sp", "tp"),
        P(None, "sp", "tp"),
        P(None, None, "tp"),
        P(None, "tp", "sp"),
    )
    return jax.shard_map(
        functools.partial(on_device, SP, TP),
        mesh=mesh, in_specs=in_specs, out_specs=P("sp", "tp"), check_vma=False,
    )
```

```python
import functools

import jax
import jax.numpy as jnp
from jax import lax
from jax.experimental import pallas as pl
from jax.experimental.pallas import tpu as pltpu
from jax.sharding import PartitionSpec as P

EPSILON = 1e-06
MESH = pl.DeviceIdType.MESH
F32 = jnp.float32
BF16 = jnp.bfloat16


def kernel(
    dims, stream, gain, w_value, w_inner, w_outer, taps, w_output, out,
    win, wout, held, normed, mix, outer, gated, tsend, s1, r1, r2a, r2b, t3a, t3b,
    r3a, r3b, tail, halo, send_sems, w_recv, swap_recv, local_sems, ag_recv, rs_recv,
):
    L, SP, TP, D, T, kb, nb, cb = dims
    Z = SP // 2
    half = T // 2
    sp, tp = lax.axis_index("sp"), lax.axis_index("tp")
    z, x = sp // 2, lax.rem(sp, 2)
    y, c = tp // 2, lax.rem(tp, 2)
    x_dev = (sp + 1 - 2 * x, tp)
    y_dev = (sp, tp + 2 - 4 * y)
    c_dev = (sp, tp + 1 - 2 * c)
    up_dev = (sp + 2, tp)
    down_dev = (sp - 2, tp)
    has_up, has_down = z < Z - 1, z > 0

    first = (2 * z >= Z).astype(jnp.int32)
    sends = []

    def make(src, dst, recv, dev):
        slot = len(sends)
        copy = lambda: pltpu.make_async_remote_copy(
            src_ref=src(), dst_ref=dst(), send_sem=send_sems.at[slot], recv_sem=recv(),
            device_id=dev, device_id_type=MESH)
        return copy

    def send(src, dst, recv, dev):
        copy = make(lambda: src, lambda: dst, lambda: recv, dev)
        sends.append((None, copy))
        copy().start()
        return copy

    def await_recv(ref, sem, dev=x_dev):
        pltpu.make_async_remote_copy(
            src_ref=ref, dst_ref=ref, send_sem=send_sems.at[0], recv_sem=sem,
            device_id=dev, device_id_type=MESH).wait_recv()

    w_in = (w_value, w_inner, w_outer)
    col = lambda q: pl.ds(pl.multiple_of(q * nb, nb), nb)
    krow = lambda s: pl.ds(pl.multiple_of(s * kb, kb), kb)

    def parts(l, s):
        return (win.at[l, :, krow(s), :], wout.at[l, s])

    def swap_parts(l, q, s):
        for i in range(3):
            yield i, w_in[i].at[l, :, col(q)], win.at[l, i, krow(s), :]
        yield 3, w_output.at[l, col(q), :], wout.at[l, s]

    def local_copies(l):
        return [pltpu.make_async_copy(src, dst, local_sems.at[l, i])
                for i, src, dst in swap_parts(l, x, sp)]

    def swap_start(l):
        for i, src, dst in swap_parts(l, 1 - x, sp):
            send(src, dst, swap_recv.at[l, i], x_dev)

    def swap_wait(l, part):
        for i, src, dst in swap_parts(l, x, x_dev[0]):
            if (i == 3) == (part == OUT):
                await_recv(dst, swap_recv.at[l, i])

    middle = jnp.logical_and(has_up, has_down)
    ends = jnp.logical_not(middle)
    IN, OUT = 0, 1

    def relay(l, part, h, picks=None, only=None):
        for p in (picks or (x, 1 - x)):
            for sign, neighbour, dev in ((-1, has_up, up_dev), (1, has_down, down_dev)):
                origin = z + sign * h
                cond = jnp.logical_and(neighbour, jnp.logical_and(origin >= 0, origin < Z))
                if only is not None:
                    cond = jnp.logical_and(cond, only)
                s = 2 * origin + p

                def copy(s=s, dev=dev, slot=len(sends)):
                    ref = parts(l, s)[part]
                    return pltpu.make_async_remote_copy(
                        src_ref=ref, dst_ref=ref, send_sem=send_sems.at[slot],
                        recv_sem=w_recv.at[l, s, part], device_id=dev, device_id_type=MESH)
                sends.append((cond, copy))

                @pl.when(cond)
                def _(s=s, copy=copy, dev=dev):
                    if h > 0:
                        await_recv(parts(l, s)[part], w_recv.at[l, s, part], dev)
                    copy().start()

    def weights_done(l, part, near=None):
        for d in range(1, Z):
            for sign, neighbour in ((-1, has_up), (1, has_down)):
                origin = z + sign * d
                inside = jnp.logical_and(origin >= 0, origin < Z)
                if near is not None:
                    same = (2 * origin >= Z) == (first == 1)
                    inside = jnp.logical_and(inside, same if near else jnp.logical_not(same))

                @pl.when(jnp.logical_and(jnp.logical_not(neighbour), inside))
                def _(origin=origin):
                    for p in range(2):
                        s = 2 * origin + p
                        await_recv(parts(l, s)[part], w_recv.at[l, s, part])

    rows_of = {0: pl.ds(0, half), 1: pl.ds(half, half)}

    def gather_start(l):
        for hf, dev in ((1, x_dev), (0, y_dev), (0, x_dev), (1, y_dev)):
            ref = held.at[l, tp, x, rows_of[hf], :]
            send(ref, ref, ag_recv.at[l, tp, x, hf], dev)
        ref = held.at[l, tp, x]
        send(ref, ref, ag_recv.at[l, tp, x, 0], c_dev)

    def gather_rest(l):
        ox, oy = 1 - x, y_dev[1]

        def got(j, xx, hf):
            await_recv(held.at[l, j, xx, rows_of[hf], :], ag_recv.at[l, j, xx, hf])

        got(tp, ox, 1)
        ref = held.at[l, tp, ox, rows_of[1], :]
        send(ref, ref, ag_recv.at[l, tp, ox, 1], y_dev)
        got(oy, x, 0)
        ref = held.at[l, oy, x, rows_of[0], :]
        send(ref, ref, ag_recv.at[l, oy, x, 0], x_dev)
        for j, xx, waits in ((tp, ox, (0,)), (oy, x, (1,)), (oy, ox, (0, 1))):
            for hf in waits:
                got(j, xx, hf)
            ref = held.at[l, j, xx]
            send(ref, ref, ag_recv.at[l, j, xx, 0], c_dev)
        cj, coy = c_dev[1], c_dev[1] + 2 - 4 * y
        for j in (cj, coy):
            for xx in range(2):
                await_recv(held.at[l, j, xx], ag_recv.at[l, j, xx, 0])

    nr = min(128, T)
    per = T // nr

    def normalize(l):
        def body(i, carry):
            xx, r = i // per, lax.rem(i, per)
            rows = pl.ds(pl.multiple_of(r * nr, nr), nr)
            blocks = [held[l, j, xx, rows, :].astype(F32) for j in range(TP)]
            total = sum(jnp.sum(b * b, axis=-1, keepdims=True) for b in blocks)
            scale = lax.rsqrt(total * (1.0 / D) + EPSILON)
            to = pl.ds(pl.multiple_of(i * nr, nr), nr)
            for j in range(TP):
                g = gain[l:l + 1, j * cb:(j + 1) * cb]
                normed[to, j * cb:(j + 1) * cb] = (blocks[j] * scale * g).astype(BF16)
            return carry
        lax.fori_loop(0, 2 * per, body, 0)

    pb = T
    mb = min(256, T)
    mper = T // mb

    def project(l):
        def body(i, carry):
            rows = pl.ds(pl.multiple_of(i * pb, pb), pb)
            n = normed[rows, :]
            v = jnp.dot(n, win[l, 0], preferred_element_type=F32)
            g = jnp.dot(n, win[l, 1], preferred_element_type=F32)
            mix[pl.ds(pl.multiple_of(16 + i * pb, 16), pb), :] = (g * v).astype(BF16).astype(F32)
            outer[rows, :] = jnp.dot(n, win[l, 2], preferred_element_type=F32)
            return carry
        lax.fori_loop(0, 2, body, 0)
        tail[l] = mix[2 * T:2 * T + 16, :].astype(BF16)
        copy = make(lambda: tail.at[l], lambda: halo.at[l], lambda: rs_recv.at[l, 0], up_dev)
        sends.append((has_up, copy))

        @pl.when(has_up)
        def _():
            copy().start()

    def w_block(l, j):
        per_tp = SP // TP
        return jnp.concatenate([wout[l, j * per_tp + q] for q in range(per_tp)], axis=1)

    def convolve(l):
        mix[0:16, :] = jnp.zeros((16, nb), F32)

        @pl.when(has_down)
        def _():
            await_recv(halo.at[l], rs_recv.at[l, 0])
            mix[0:16, :] = halo[l].astype(F32)

        tap = taps[l, :, col(x)]

        def body(i, carry):
            m = mix[pl.ds(pl.multiple_of(8 + i * mb, 8), mb + 8), :]
            conv = tap[0:1] * m[6:6 + mb] + tap[1:2] * m[7:7 + mb] + tap[2:3] * m[8:8 + mb]
            rows = pl.ds(pl.multiple_of(i * mb, mb), mb)
            gated[rows, :] = (outer[rows, :] * conv).astype(BF16)
            return carry
        lax.fori_loop(0, 2 * mper, body, 0)

    def outputs(l, yj, target, core, finish):
        w = w_block(l, 2 * yj + core)

        def body(i, carry):
            g = gated[pl.ds(pl.multiple_of(i * pb, pb), pb), :]
            t = jnp.dot(g, w, preferred_element_type=F32).astype(BF16)
            if finish:
                t = (t.astype(F32) + r1[l, yj, i].astype(F32)).astype(BF16)
            target[l, yj, i] = t
            return carry
        if finish:
            await_recv(r1.at[l, yj], rs_recv.at[l, 1 + yj])
        lax.fori_loop(0, 2, body, 0)
        if not finish:
            send(tsend.at[l, yj], r1.at[l, yj], rs_recv.at[l, 1 + yj], c_dev)

    def output_group(l, yj):
        A, B = rows_of[0], rows_of[1]
        outputs(l, yj, tsend, 1 - c, False)
        outputs(l, yj, s1, c, True)
        send(s1.at[l, yj, 1 - x, A, :], r2a.at[l, yj], rs_recv.at[l, 3 + yj], x_dev)
        other = yj != y
        for xj in (1 - x, x):
            copy = make(
                lambda xj=xj: s1.at[l, yj, xj, B, :], lambda xj=xj: r2b.at[l, xj],
                lambda xj=xj: rs_recv.at[l, 5 + xj], y_dev)
            sends.append((other, copy))

            @pl.when(other)
            def _(copy=copy):
                copy().start()

    def f(ref):
        return ref.astype(F32)

    def reduce(l, store):
        A, B = rows_of[0], rows_of[1]
        await_recv(r2a.at[l, 1 - y], rs_recv.at[l, 4 - y])
        t3a[l] = (f(s1[l, 1 - y, x, A, :]) + f(r2a[l, 1 - y])).astype(BF16)
        send(t3a.at[l], r3a.at[l], rs_recv.at[l, 7], y_dev)
        await_recv(r2b.at[l, 1 - x], rs_recv.at[l, 6 - x])
        t3b[l] = (f(s1[l, y, 1 - x, B, :]) + f(r2b[l, 1 - x])).astype(BF16)
        send(t3b.at[l], r3b.at[l], rs_recv.at[l, 8], x_dev)
        await_recv(r2a.at[l, y], rs_recv.at[l, 3 + y])
        await_recv(r3a.at[l], rs_recv.at[l, 7])
        branch = f(s1[l, y, x, A, :]) + f(r2a[l, y]) + f(r3a[l])
        store(A, (f(held[l, tp, x, A, :]) + branch).astype(BF16))
        await_recv(r2b.at[l, x], rs_recv.at[l, 5 + x])
        await_recv(r3b.at[l], rs_recv.at[l, 8])
        branch = f(s1[l, y, x, B, :]) + f(r2b[l, x]) + f(r3b[l])
        store(B, (f(held[l, tp, x, B, :]) + branch).astype(BF16))

    copies = [local_copies(l) for l in range(L)]
    for group in copies:
        for copy in group:
            copy.start()
    held[0, tp, x] = stream[...]

    barrier = pltpu.get_barrier_semaphore()
    for dev in (x_dev, y_dev, c_dev):
        pl.semaphore_signal(barrier, inc=1, device_id=dev, device_id_type=MESH)
    for cond, dev in ((has_up, up_dev), (has_down, down_dev)):
        @pl.when(cond)
        def _(dev=dev):
            pl.semaphore_signal(barrier, inc=1, device_id=dev, device_id_type=MESH)
    peers = 3 + has_up.astype(jnp.int32) + has_down.astype(jnp.int32)
    pl.semaphore_wait(barrier, peers)

    swap_start(0)
    for copy in copies[0][:3]:
        copy.wait()
    relay(0, IN, 0, (x,))
    copies[0][3].wait()
    relay(0, OUT, 0, (x,))
    gather_start(0)
    swap_wait(0, IN)
    relay(0, IN, 0, (1 - x,))
    swap_wait(0, OUT)
    relay(0, OUT, 0, (1 - x,), only=ends)
    if Z > 2:
        relay(0, IN, 1)
    gather_rest(0)
    for l in range(1, L):
        swap_start(l)
    for h in range(2, Z - 1):
        relay(0, IN, h)
    relay(0, OUT, 0, (1 - x,), only=middle)
    normalize(0)
    for l in range(1, L):
        for copy in copies[l]:
            copy.wait()
        swap_wait(l, IN)
        swap_wait(l, OUT)
        relay(l, IN, 0, only=ends)
        relay(l, OUT, 0, only=ends)
    for l in range(L):
        weights_done(l, IN)
        project(l)
        for h in range(1, Z - 1):
            relay(l, OUT, h)
        if l + 1 < L:
            relay(l + 1, IN, 0, only=middle)
        convolve(l)
        weights_done(l, OUT, True)
        output_group(l, first)
        weights_done(l, OUT, False)
        output_group(l, 1 - first)
        if l + 1 < L:
            def store(rows, value, l=l):
                held[l + 1, tp, x, rows, :] = value
            if Z > 2:
                relay(l + 1, IN, 1)
            reduce(l, store)
            gather_start(l + 1)
            for h in range(2, Z - 1):
                relay(l + 1, IN, h)
            gather_rest(l + 1)
            relay(l + 1, OUT, 0, only=middle)
            normalize(l + 1)
        else:
            def store(rows, value):
                out[rows, :] = value
            reduce(l, store)

    for cond, copy in sends:
        if cond is None:
            copy().wait_send()
        else:
            @pl.when(cond)
            def _(copy=copy):
                copy().wait_send()


def on_device(SP, TP, stream, norm_gain, w_value, w_inner, w_outer, conv_taps, w_output):
    L, kb, cb = w_value.shape
    T, D = stream.shape[0], norm_gain.shape[1]
    nb, Z = cb // 2, SP // 2
    dims = (L, SP, TP, D, T, kb, nb, cb)
    vmem = pl.BlockSpec(memory_space=pltpu.VMEM)
    hbm = pl.BlockSpec(memory_space=pl.ANY)
    half = T // 2
    n_sends = L * (4 + 8 * max(Z - 1, 1) + 8 + 10 + 13)
    return pl.pallas_call(
        functools.partial(kernel, dims),
        out_shape=jax.ShapeDtypeStruct((T, cb), BF16),
        in_specs=[vmem, vmem, hbm, hbm, hbm, vmem, hbm],
        out_specs=vmem,
        scratch_shapes=[
            pltpu.VMEM((L, 3, D, nb), BF16),
            pltpu.VMEM((L, SP, nb, kb), BF16),
            pltpu.VMEM((L, TP, 2, T, cb), BF16),
            pltpu.VMEM((2 * T, D), BF16),
            pltpu.VMEM((2 * T + 16, nb), F32),
            pltpu.VMEM((2 * T, nb), F32),
            pltpu.VMEM((2 * T, nb), BF16),
            pltpu.VMEM((L, 2, 2, T, cb), BF16),
            pltpu.VMEM((L, 2, 2, T, cb), BF16),
            pltpu.VMEM((L, 2, 2, T, cb), BF16),
            pltpu.VMEM((L, 2, half, cb), BF16),
            pltpu.VMEM((L, 2, half, cb), BF16),
            pltpu.VMEM((L, half, cb), BF16),
            pltpu.VMEM((L, half, cb), BF16),
            pltpu.VMEM((L, half, cb), BF16),
            pltpu.VMEM((L, half, cb), BF16),
            pltpu.VMEM((L, 16, nb), BF16),
            pltpu.VMEM((L, 16, nb), BF16),
            pltpu.SemaphoreType.DMA((n_sends,)),
            pltpu.SemaphoreType.DMA((L, SP, 2)),
            pltpu.SemaphoreType.DMA((L, 4)),
            pltpu.SemaphoreType.DMA((L, 4)),
            pltpu.SemaphoreType.DMA((L, TP, 2, 2)),
            pltpu.SemaphoreType.DMA((L, 9)),
        ],
        compiler_params=pltpu.CompilerParams(
            collective_id=0, has_side_effects=True, vmem_limit_bytes=60 * 1024 * 1024
        ),
    )(stream, norm_gain, w_value, w_inner, w_outer, conv_taps, w_output)


def solution(mesh):
    SP, TP = mesh.shape["sp"], mesh.shape["tp"]
    in_specs = (
        P("sp", "tp"),
        P(),
        P(None, "sp", "tp"),
        P(None, "sp", "tp"),
        P(None, "sp", "tp"),
        P(None, None, "tp"),
        P(None, "tp", "sp"),
    )
    return jax.shard_map(
        functools.partial(on_device, SP, TP),
        mesh=mesh, in_specs=in_specs, out_specs=P("sp", "tp"), check_vma=False,
    )
```
